256 devices in a mesh: grp: 4 (over y, x), ep: 32 (over z), tp: 2 (over core).
Axes of the slice: x: 2, y: 2, z: 32, core: 2. Of those that a mesh axis runs over, the one named last changes fastest.
The devices are a block of a 4x16x32 slice.
Arguments:
- tokens: bfloat16 [4096, 2048], P(('grp', 'ep')), parts along dimension 0, may hold values from -6 to 6
- norm_gain: float32 [2048], replicated, may hold values from 0.1 to 1.9
- group_prob: float32 [4096], P(('grp', 'ep')), parts along dimension 0, may hold values from 0.5 to 1
- route_logits: float32 [4096, 4], P(('grp', 'ep')), parts along dimension 0, may hold values from -6 to 6
- expert_ids: int32 [4096, 4], P(('grp', 'ep')), parts along dimension 0, may hold values from 0 to 31, as said below
- w_gate: bfloat16 [32, 2048, 512], P('ep', None, 'tp'), may hold values from -0.125 to 0.125
- w_up: bfloat16 [32, 2048, 512], P('ep', None, 'tp'), may hold values from -0.125 to 0.125
- w_down: bfloat16 [32, 512, 2048], P('ep', 'tp'), may hold values from -0.25 to 0.25
Outputs:
- mixed: bfloat16 [4096, 2048], P(('grp', 'ep')), parts along dimension 0
The draws below stay inside these ranges and needn't reach their ends.
There are 4 independent parts, one for each index of `grp`. The reference program is written for one: setup_inputs(seed, part) draws one part's arguments, and reference() takes and returns one part's arrays. A program takes and returns all parts, laid end to end along the dimension named above; an argument that names none is the same for every part. Nothing has to cross between parts.
Inputs may be any that keep to these rules, and one draw needn't show every extreme that they name: `expert_ids`: each token names 4 different experts, all inside one group of 16 consecutive experts. Of the 32 tokens of one index of ep, exactly 16 lie in each group, so at most 16 of them name any one expert; in every draw some expert is named by 16 tokens of every index of ep.
All inputs are finite; a program needn't handle non-finite values.
Results may differ from the reference program's by a relative error of at most 0.0077.
Values may be sent and summed in bfloat16 or wider, within the bound.
No kernel may reach another device: no remote copies, remote signals or barrier semaphores. Data moves between devices by JAX's collectives and lax.ppermute only.
A program may use at most 64 MiB of HBM per device.

```python
import jax
import jax.numpy as jnp
from jax import lax

D = 2048
FF = 512
GROUPS = 2
TOP_K = 4
TOK_DEV = 32
EXPERTS = 32
GROUP_SIZE = 16
TOKENS = 1024
N_TP = 2


def draw_expert_ids(key, part):
    blocks = TOKENS // TOK_DEV
    keys = jax.random.split(jax.random.fold_in(key, 7), 5)
    labels = jnp.arange(TOK_DEV, dtype=jnp.int32) % GROUPS
    perms = jax.vmap(lambda k: jax.random.permutation(k, labels))(jax.random.split(keys[0], blocks))
    common_hot = jax.random.randint(keys[1], (), 0, GROUP_SIZE)
    hot = jax.random.randint(keys[2], (blocks, GROUPS), 0, GROUP_SIZE)
    hot = hot.at[:, 0].set(common_hot)
    bias = jax.random.randint(keys[3], (GROUPS, GROUP_SIZE), 0, 4) * 32
    noise = jax.random.randint(keys[4], (blocks, TOK_DEV, GROUP_SIZE), 0, 64)
    local = jnp.arange(GROUP_SIZE, dtype=jnp.int32)
    token_bias = bias[perms]
    token_hot = jnp.take_along_axis(hot, perms, axis=1)
    boost = (local[None, None, :] == token_hot[:, :, None]).astype(jnp.int32) * 100000
    scores = (noise + token_bias + boost) * GROUP_SIZE + local[None, None, :]
    unused, picked = lax.top_k(scores, TOP_K)
    ids = perms[:, :, None] * GROUP_SIZE + picked.astype(jnp.int32)
    return ids.reshape(TOKENS, TOP_K).astype(jnp.int32)


def levels(own_key, shape, pieces, low, largest):
    factor_of, own = 1.0, jax.random.fold_in(own_key, 6)
    for position, shards_of in pieces:
        heights = jnp.exp(jax.random.uniform(jax.random.fold_in(own, position), (shards_of,), jnp.float32, low / len(pieces), largest / len(pieces)))
        factor_of = factor_of * jnp.repeat(heights, shape[position] // shards_of).reshape([-1 if axis == position else 1 for axis in range(len(shape))])
    return factor_of


def normal_values(rng, dims, deviation, limit, cuts=(), held_as=jnp.bfloat16):
    factor_of = levels(rng, dims, cuts, -0.22, 0.18) if cuts else 1.0
    drawn = jax.random.normal(rng, dims, jnp.float32) * deviation * factor_of
    return jnp.minimum(jnp.maximum(drawn, -limit), limit).astype(held_as)


def setup_inputs(seed: int = 0, part: int = 0) -> dict:
    arg_keys = jax.random.split(jax.random.key(seed), 9)
    part_keys = jax.random.split(jax.random.fold_in(arg_keys[8], part), 9)
    return {
        "tokens": normal_values(part_keys[0], (TOKENS, D), 1.0, 6.0, ((0, 32),)),
        "norm_gain": jnp.clip(1.0 + 0.18 * jax.random.normal(arg_keys[1], (D,), jnp.float32), 0.1, 1.9),
        "group_prob": jnp.clip(0.5 + 0.5 * jax.random.uniform(part_keys[2], (TOKENS,), jnp.float32) ** levels(part_keys[2], (TOKENS,), ((0, 32),), -0.2, 0.2), 0.5, 1.0),
        "route_logits": normal_values(part_keys[3], (TOKENS, TOP_K), 1.0, 6.0, ((0, 32),), jnp.float32),
        "expert_ids": draw_expert_ids(jax.random.fold_in(jax.random.fold_in(arg_keys[8], part), 71), part),
        "w_gate": normal_values(arg_keys[5], (EXPERTS, D, FF), D ** -0.5, 0.125, ((0, 32), (2, 2))),
        "w_up": normal_values(arg_keys[6], (EXPERTS, D, FF), D ** -0.5, 0.125, ((0, 32), (2, 2))),
        "w_down": normal_values(arg_keys[7], (EXPERTS, FF, D), FF ** -0.5, 0.25, ((0, 32), (1, 2))),
    }


def reference(tokens, norm_gain, group_prob, route_logits, expert_ids, w_gate, w_up, w_down):
    values = tokens.astype(jnp.float32)
    scale = lax.rsqrt(lax.optimization_barrier(jnp.mean(values * values, axis=-1, keepdims=True)) + 1e-06)
    normed = (values * scale * norm_gain).astype(jnp.bfloat16)
    expw = jnp.exp(route_logits)
    route_w = group_prob[:, None] * expw / lax.optimization_barrier(jnp.sum(expw, axis=-1, keepdims=True))
    block = FF // N_TP

    def one_expert(acc, inputs):
        gate_m, up_m, down_m, index = inputs
        gate = jnp.dot(normed, gate_m, preferred_element_type=jnp.float32)
        up = jnp.dot(normed, up_m, preferred_element_type=jnp.float32)
        act = (jax.nn.silu(gate) * up).astype(jnp.bfloat16)
        total = jnp.zeros((normed.shape[0], normed.shape[1]), jnp.float32)
        for piece in range(N_TP):
            part = jnp.dot(act[:, piece * block:(piece + 1) * block], down_m[piece * block:(piece + 1) * block], preferred_element_type=jnp.float32).astype(jnp.bfloat16)
            total = total + lax.optimization_barrier(part).astype(jnp.float32)
        expert_out = lax.optimization_barrier(total.astype(jnp.bfloat16)).astype(jnp.float32)
        weight = lax.optimization_barrier(jnp.sum(route_w * (expert_ids == index).astype(jnp.float32), axis=1))
        return (acc + weight[:, None] * expert_out, None)
    start = jnp.zeros((normed.shape[0], normed.shape[1]), jnp.float32)
    experts = jnp.arange(EXPERTS, dtype=jnp.int32)
    acc, unused = lax.scan(one_expert, start, (w_gate, w_up, w_down, experts))
    return acc.astype(jnp.bfloat16)
```

```python
import functools

import jax
import jax.numpy as jnp
from jax import lax
from jax.experimental import pallas as pl
from jax.experimental.pallas import tpu as pltpu
from jax.sharding import PartitionSpec as P


LANES = 128
FAR = 8
STEPS = 4
CLASSES = {0: (4, 4), 8: (3, 4), 16: (3, 3), -8: (4, 3)}


def prepare_kernel(tokens, gain, prob, logits, ids, unit):
    rows, width = unit.shape
    model = tokens.shape[1]
    core = lax.axis_index("tp")
    values = tokens[pl.ds(pl.multiple_of(core * rows, rows), rows), :].astype(jnp.float32)
    scale = lax.rsqrt(jnp.mean(values * values, axis=-1, keepdims=True) + 1e-06)
    unit[:, :model] = (values * scale * gain[...]).astype(jnp.bfloat16)
    expw = jnp.exp(logits[...])
    route_w = prob[...] * expw / jnp.sum(expw, axis=0, keepdims=True)
    picks, count = expw.shape
    experts = lax.axis_size("ep")
    expert = lax.broadcasted_iota(jnp.int32, (experts, count), 0)
    dense = jnp.zeros((experts, count), jnp.float32)
    for k in range(picks):
        dense += jnp.where(ids[k : k + 1, :] == expert, route_w[k : k + 1, :], 0.0)
    high = dense.astype(jnp.bfloat16).astype(jnp.float32)
    low = dense - high
    table = jnp.concatenate(
        [high, low, jnp.zeros((width - model - 2 * experts, count), jnp.float32)], axis=0
    ).astype(jnp.bfloat16)
    row = lax.broadcasted_iota(jnp.int32, (rows, count), 0) + core * rows
    chosen = (lax.broadcasted_iota(jnp.int32, (rows, count), 1) == row).astype(jnp.bfloat16)
    unit[:, model:] = lax.dot_general(
        chosen, table, (((1,), (1,)), ((), ())), preferred_element_type=jnp.float32
    ).astype(jnp.bfloat16)


def expert_kernel(n, *refs):
    units, weights, outs = refs[:n], refs[n : n + 6], refs[n + 6 : 2 * n + 6]
    rows_all, weight_all, part_all = refs[2 * n + 6 :]
    rows, width = units[0].shape
    model = rows_all.shape[1]
    me = lax.axis_index("ep")
    experts = lax.axis_size("ep")
    lane = lax.broadcasted_iota(jnp.int32, (rows, width - model), 1)
    mine = (lane == me) | (lane == me + experts)
    for k in range(n):
        at = slice(k * rows, (k + 1) * rows)
        rows_all[at, :] = units[k][:, :model]
        own = jnp.where(mine, units[k][:, model:].astype(jnp.float32), 0.0)
        weight_all[at, :] = jnp.broadcast_to(
            jnp.sum(own, axis=1, keepdims=True), (rows, width - model)
        )

    step = n * rows // STEPS

    def block(x, gate_w, up_w, down_w):
        gate = jnp.dot(x, gate_w[0], preferred_element_type=jnp.float32)
        up = jnp.dot(x, up_w[0], preferred_element_type=jnp.float32)
        act = (gate / (1.0 + jnp.exp(-gate)) * up).astype(jnp.bfloat16)
        return jnp.dot(act, down_w[0], preferred_element_type=jnp.float32).astype(jnp.bfloat16)

    def some(i, carry):
        at = pl.ds(pl.multiple_of(i * step, step), step)
        x = rows_all[at, :]
        part_all[at, :] = block(x, *weights[:3])
        other = block(x, *weights[3:]).astype(jnp.float32)
        total = (part_all[at, :].astype(jnp.float32) + other).astype(jnp.bfloat16)
        weighted = total.astype(jnp.float32) * weight_all[at, :1]
        part_all[at, :] = weighted.astype(jnp.bfloat16)
        return carry

    lax.fori_loop(0, STEPS, some, 0)
    for k in range(n):
        outs[k][...] = part_all[k * rows : (k + 1) * rows, :]


VMEM = pl.BlockSpec(memory_space=pltpu.VMEM)


def prepare(tokens, norm_gain, group_prob, route_logits, expert_ids):
    rows = tokens.shape[0] // lax.axis_size("tp")
    return pl.pallas_call(
        prepare_kernel,
        out_shape=jax.ShapeDtypeStruct((rows, tokens.shape[1] + LANES), jnp.bfloat16),
        in_specs=[VMEM] * 5,
        out_specs=VMEM,
        name="prepare",
    )(tokens, norm_gain[None, :], group_prob[None, :], route_logits.T, expert_ids.T)


def expert(units, weights):
    n = len(units)
    rows, width = units[0].shape
    model = width - LANES
    return pl.pallas_call(
        functools.partial(expert_kernel, n),
        out_shape=[jax.ShapeDtypeStruct((rows, model), jnp.bfloat16)] * n,
        in_specs=[VMEM] * (n + 6),
        out_specs=[VMEM] * n,
        scratch_shapes=[
            pltpu.VMEM((n * rows, model), jnp.bfloat16),
            pltpu.VMEM((n * rows, LANES), jnp.float32),
            pltpu.VMEM((n * rows, model), jnp.bfloat16),
        ],
        compiler_params=pltpu.CompilerParams(vmem_limit_bytes=24 * 1024 * 1024),
        name="expert",
    )(*units, *weights)


def moved(array, shift):
    n = lax.axis_size("ep")
    return lax.ppermute(array, "ep", [(i, (i + shift) % n) for i in range(n)])


def turned(array, shift):
    n, cores = lax.axis_size("ep"), lax.axis_size("tp")
    pairs = []
    for i in range(n):
        for core in range(cores):
            to = (i + (shift if core == 0 else -shift)) % n
            pairs.append((i * cores + core, to * cores + core))
    return lax.ppermute(array, ("ep", "tp"), pairs)


def added(*pieces):
    total = pieces[0].astype(jnp.float32)
    for piece in pieces[1:]:
        total = total + piece.astype(jnp.float32)
    return total.astype(jnp.bfloat16)


def gather(unit, first):
    below, above = moved(unit, FAR), moved(unit, -FAR)
    across = turned(jnp.where(first, below, above), FAR)
    held = {}
    for base, at in ((0, unit), (-FAR, below), (FAR, above), (2 * FAR, across)):
        left, right = CLASSES[base]
        held[base, 0] = at
        for off in range(1, max(left, right) + 1):
            if off <= right:
                held[base, off] = moved(held[base, off - 1], -1)
            if off <= left:
                held[base, -off] = moved(held[base, 1 - off], 1)
    return held


def combine(held, first):
    sums = {}
    for base in (2 * FAR, FAR, -FAR, 0):
        left, right = CLASSES[base]
        up, down = held[base, right], held[base, -left]
        for off in range(right - 1, 0, -1):
            up = added(moved(up, 1), held[base, off])
        for off in range(left - 1, 0, -1):
            down = added(moved(down, -1), held[base, -off])
        sums[base] = (held[base, 0], moved(up, 1), moved(down, -1))
    across = turned(added(*sums[2 * FAR]), -FAR).astype(jnp.float32)
    zero = jnp.zeros_like(across)
    above = added(*sums[FAR], jnp.where(first, zero, across))
    below = added(*sums[-FAR], jnp.where(first, across, zero))
    return added(*sums[0], moved(above, FAR), moved(below, -FAR))


def shards(tokens, norm_gain, group_prob, route_logits, expert_ids, w_gate, w_up, w_down):
    first = lax.axis_index("tp") == 0
    own = (w_gate, w_up, w_down)
    other = tuple(lax.ppermute(w, "tp", [(0, 1), (1, 0)]) for w in own)
    unit = prepare(tokens, norm_gain, group_prob, route_logits, expert_ids)
    held = gather(unit, first)
    keys = sorted(held)
    outs = expert([held[key] for key in keys], own + other)
    mixed = combine(dict(zip(keys, outs)), first)
    return lax.all_gather(mixed, "tp", axis=0, tiled=True)


def solution(mesh):
    in_specs = (
        P(("grp", "ep"), None),
        P(),
        P(("grp", "ep")),
        P(("grp", "ep"), None),
        P(("grp", "ep"), None),
        P("ep", None, "tp"),
        P("ep", None, "tp"),
        P("ep", "tp", None),
    )
    out_specs = P(("grp", "ep"), None)
    return jax.shard_map(shards, mesh=mesh, in_specs=in_specs, out_specs=out_specs, check_vma=False)
```

```python
import functools

import jax
import jax.numpy as jnp
from jax import lax
from jax.experimental import pallas as pl
from jax.experimental.pallas import tpu as pltpu
from jax.sharding import PartitionSpec as P


LANES = 128
STEPS = 4
BASES = (0, 7, 14)
LAST = 16


def prepare_kernel(tokens, gain, prob, logits, ids, unit):
    rows, width = unit.shape
    model = tokens.shape[1]
    values = tokens[...].astype(jnp.float32)
    scale = lax.rsqrt(jnp.mean(values * values, axis=-1, keepdims=True) + 1e-06)
    unit[:, :model] = (values * scale * gain[...]).astype(jnp.bfloat16)
    expw = jnp.exp(logits[...])
    route_w = prob[...] * expw / jnp.sum(expw, axis=0, keepdims=True)
    picks, count = expw.shape
    experts = lax.axis_size("ep")
    expert = lax.broadcasted_iota(jnp.int32, (experts, count), 0)
    dense = jnp.zeros((experts, count), jnp.float32)
    for k in range(picks):
        dense += jnp.where(ids[k : k + 1, :] == expert, route_w[k : k + 1, :], 0.0)
    high = dense.astype(jnp.bfloat16).astype(jnp.float32)
    low = dense - high
    table = jnp.concatenate(
        [high, low, jnp.zeros((width - model - 2 * experts, count), jnp.float32)], axis=0
    ).astype(jnp.bfloat16)
    row = lax.broadcasted_iota(jnp.int32, (rows, count), 0)
    chosen = (lax.broadcasted_iota(jnp.int32, (rows, count), 1) == row).astype(jnp.bfloat16)
    unit[:, model:] = lax.dot_general(
        chosen, table, (((1,), (1,)), ((), ())), preferred_element_type=jnp.float32
    ).astype(jnp.bfloat16)


def pieces(n, rows, core):
    half, at = rows // 2, 0
    mine = pl.ds(pl.multiple_of(core * half, half), half)
    for k in range(n):
        some, count = (mine, half) if k in (0, n - 1) else (slice(None), rows)
        yield k, some, slice(at, at + count)
        at += count


def block(x, gate_w, up_w, down_w):
    gate = jnp.dot(x, gate_w[0], preferred_element_type=jnp.float32)
    up = jnp.dot(x, up_w[0], preferred_element_type=jnp.float32)
    act = (gate / (1.0 + jnp.exp(-gate)) * up).astype(jnp.bfloat16)
    return jnp.dot(act, down_w[0], preferred_element_type=jnp.float32).astype(jnp.bfloat16)


def chunks(total, body):
    step = total // STEPS

    def one(i, carry):
        body(pl.ds(pl.multiple_of(i * step, step), step))
        return carry

    lax.fori_loop(0, STEPS, one, 0)


def first_kernel(n, *refs):
    units, other, (rows_all, weight_all, part_all) = refs[:n], refs[n : n + 3], refs[n + 3 :]
    rows, width = units[0].shape
    total_rows, model = rows_all.shape
    me, core = lax.axis_index("ep"), lax.axis_index("tp")
    experts = lax.axis_size("ep")
    for k, some, at in pieces(n, rows, core):
        rows_all[at, :] = units[k][some, :model]
        table = units[k][some, model:].astype(jnp.float32)
        lane = lax.broadcasted_iota(jnp.int32, table.shape, 1)
        taken = jnp.where((lane == me) | (lane == me + experts), table, 0.0)
        weight_all[at, :] = jnp.broadcast_to(jnp.sum(taken, axis=1, keepdims=True), table.shape)

    def body(at):
        part_all[at, :] = block(rows_all[at, :], *other)

    chunks(total_rows, body)


def second_kernel(n, *refs):
    (rows_all, weight_all, part_all, *own), outs, mixed_all = refs[:6], refs[6 : 6 + n], refs[-1]

    def body(at):
        part = block(rows_all[at, :], *own).astype(jnp.float32)
        total = (part_all[at, :].astype(jnp.float32) + part).astype(jnp.bfloat16)
        weighted = total.astype(jnp.float32) * weight_all[at, :1]
        mixed_all[at, :] = weighted.astype(jnp.bfloat16)

    chunks(rows_all.shape[0], body)
    for k, some, at in pieces(n, outs[0].shape[0], lax.axis_index("tp")):
        if k in (0, n - 1):
            outs[k][...] = jnp.zeros_like(outs[k])
        outs[k][some, :] = mixed_all[at, :]


VMEM = pl.BlockSpec(memory_space=pltpu.VMEM)


def prepare(tokens, norm_gain, group_prob, route_logits, expert_ids):
    rows, model = tokens.shape
    return pl.pallas_call(
        prepare_kernel,
        out_shape=jax.ShapeDtypeStruct((rows, model + LANES), jnp.bfloat16),
        in_specs=[VMEM] * 5,
        out_specs=VMEM,
        name="prepare",
    )(tokens, norm_gain[None, :], group_prob[None, :], route_logits.T, expert_ids.T)


def expert(units, own, other):
    n = len(units)
    rows, width = units[0].shape
    model = width - LANES
    total = (n - 1) * rows
    params = pltpu.CompilerParams(vmem_limit_bytes=20 * 1024 * 1024)
    whole = jax.ShapeDtypeStruct((total, model), jnp.bfloat16)
    held = pl.pallas_call(
        functools.partial(first_kernel, n),
        out_shape=[whole, jax.ShapeDtypeStruct((total, LANES), jnp.float32), whole],
        in_specs=[VMEM] * (n + 3),
        out_specs=[VMEM] * 3,
        compiler_params=params,
        name="first",
    )(*units, *other)
    return pl.pallas_call(
        functools.partial(second_kernel, n),
        out_shape=[jax.ShapeDtypeStruct((rows, model), jnp.bfloat16)] * n,
        in_specs=[VMEM] * 6,
        out_specs=[VMEM] * n,
        scratch_shapes=[pltpu.VMEM((total, model), jnp.bfloat16)],
        compiler_params=params,
        name="second",
    )(*held, *own)


def turned(array, shift):
    n, cores = lax.axis_size("ep"), lax.axis_size("tp")
    pairs = []
    for i in range(n):
        for core in range(cores):
            to = (i + (shift if core == 0 else -shift)) % n
            pairs.append((i * cores + core, to * cores + core))
    return lax.ppermute(array, ("ep", "tp"), pairs)


def swapped(array):
    return lax.ppermute(array, "tp", [(0, 1), (1, 0)])


def added(*parts):
    total = parts[0].astype(jnp.float32)
    for part in parts[1:]:
        total = total + part.astype(jnp.float32)
    return total.astype(jnp.bfloat16)


def spans():
    ends = (*BASES[1:], LAST + 1)
    return [(base, end - 1) for base, end in zip(BASES, ends)]


def gather(unit):
    held = {0: unit}
    for near, far in zip(BASES, BASES[1:]):
        held[far] = turned(held[near], far - near)
    for base, last in spans():
        for at in range(base + 1, last + 1):
            held[at] = turned(held[at - 1], 1)
    return [held[at] for at in range(LAST + 1)]


def combine(outs):
    above = None
    for base, last in reversed(spans()):
        chain = outs[last]
        for at in range(last - 1, base, -1):
            chain = added(turned(chain, -1), outs[at])
        parts = [outs[base], turned(chain, -1)]
        if above is not None:
            parts.append(turned(above[1], base - above[0]))
        above = base, added(*parts)
    return above[1]


def shards(tokens, norm_gain, group_prob, route_logits, expert_ids, w_gate, w_up, w_down):
    own = (w_gate, w_up, w_down)
    other = tuple(swapped(w) for w in own)
    unit = prepare(tokens, norm_gain, group_prob, route_logits, expert_ids)
    mixed = combine(expert(gather(unit), own, other))
    return added(mixed, swapped(mixed))


def solution(mesh):
    in_specs = (
        P(("grp", "ep"), None),
        P(),
        P(("grp", "ep")),
        P(("grp", "ep"), None),
        P(("grp", "ep"), None),
        P("ep", None, "tp"),
        P("ep", None, "tp"),
        P("ep", "tp", None),
    )
    out_specs = P(("grp", "ep"), None)
    return jax.shard_map(shards, mesh=mesh, in_specs=in_specs, out_specs=out_specs, check_vma=False)
```

```python
import functools

import jax
import jax.numpy as jnp
from jax import lax
from jax.experimental import pallas as pl
from jax.experimental.pallas import tpu as pltpu
from jax.sharding import PartitionSpec as P


LANES = 128
STEPS = 4
GATHER = (0, 1, 0, 3, 4, 0, 6, 6, 8, 6, 10, 11, 10, 13, 13, 15)
GATHER_ORDER = (6, 1, 3, 10, 8, 4, 7, 13, 11, 5, 2, 15, 14, 12, 9, 16)
COMBINE = (0, 1, 1, 3, 0, 5, 6, 6, 8, 5, 10, 11, 11, 10, 14, 14)
COMBINE_ORDER = (16, 15, 13, 12, 9, 14, 11, 4, 7, 8, 10, 6, 2, 3, 5, 1)
LAST = len(GATHER)


def prepare_kernel(tokens, gain, prob, logits, ids, unit, kept):
    rows, width = unit.shape
    model = tokens.shape[1]
    values = tokens[...].astype(jnp.float32)
    scale = lax.rsqrt(jnp.mean(values * values, axis=-1, keepdims=True) + 1e-06)
    unit[:, :model] = (values * scale * gain[...]).astype(jnp.bfloat16)
    expw = jnp.exp(logits[...])
    route_w = prob[...] * expw / jnp.sum(expw, axis=0, keepdims=True)
    picks, count = expw.shape
    experts = lax.axis_size("ep")
    expert = lax.broadcasted_iota(jnp.int32, (experts, count), 0)
    dense = jnp.zeros((experts, count), jnp.float32)
    for k in range(picks):
        dense += jnp.where(ids[k : k + 1, :] == expert, route_w[k : k + 1, :], 0.0)
    high = dense.astype(jnp.bfloat16).astype(jnp.float32)
    low = dense - high
    table = jnp.concatenate(
        [high, low, jnp.zeros((width - model - 2 * experts, count), jnp.float32)], axis=0
    ).astype(jnp.bfloat16)
    row = lax.broadcasted_iota(jnp.int32, (rows, count), 0)
    chosen = (lax.broadcasted_iota(jnp.int32, (rows, count), 1) == row).astype(jnp.bfloat16)
    unit[:, model:] = lax.dot_general(
        chosen, table, (((1,), (1,)), ((), ())), preferred_element_type=jnp.float32
    ).astype(jnp.bfloat16)
    kept[...] = unit[...]


def pieces(n, rows, core):
    half, at = rows // 2, 0
    mine = pl.ds(pl.multiple_of(core * half, half), half)
    for k in range(n):
        some, count = (mine, half) if k in (0, n - 1) else (slice(None), rows)
        yield k, some, slice(at, at + count)
        at += count


def block(x, gate_w, up_w, down_w):
    gate = jnp.dot(x, gate_w[0], preferred_element_type=jnp.float32)
    up = jnp.dot(x, up_w[0], preferred_element_type=jnp.float32)
    act = (gate / (1.0 + jnp.exp(-gate)) * up).astype(jnp.bfloat16)
    return jnp.dot(act, down_w[0], preferred_element_type=jnp.float32).astype(jnp.bfloat16)


def chunks(total, body):
    step = total // STEPS

    def one(i, carry):
        body(pl.ds(pl.multiple_of(i * step, step), step))
        return carry

    lax.fori_loop(0, STEPS, one, 0)


def first_kernel(n, *refs):
    units, other, (rows_all, weight_all, part_all) = refs[:n], refs[n : n + 3], refs[n + 3 :]
    rows, _ = units[0].shape
    total_rows, model = rows_all.shape
    me, core = lax.axis_index("ep"), lax.axis_index("tp")
    experts = lax.axis_size("ep")
    for k, some, at in pieces(n, rows, core):
        rows_all[at, :] = units[k][some, :model]
        table = units[k][some, model:].astype(jnp.float32)
        lane = lax.broadcasted_iota(jnp.int32, table.shape, 1)
        taken = jnp.where((lane == me) | (lane == me + experts), table, 0.0)
        weight_all[at, :] = jnp.broadcast_to(jnp.sum(taken, axis=1, keepdims=True), table.shape)

    def body(at):
        part_all[at, :] = block(rows_all[at, :], *other)

    chunks(total_rows, body)


def second_kernel(n, *refs):
    (rows_all, weight_all, part_all, *own), outs, mixed_all = refs[:6], refs[6 : 6 + n], refs[-1]

    def body(at):
        part = block(rows_all[at, :], *own).astype(jnp.float32)
        total = (part_all[at, :].astype(jnp.float32) + part).astype(jnp.bfloat16)
        weighted = total.astype(jnp.float32) * weight_all[at, :1]
        mixed_all[at, :] = weighted.astype(jnp.bfloat16)

    chunks(rows_all.shape[0], body)
    for k, some, at in pieces(n, outs[0].shape[0], lax.axis_index("tp")):
        if k in (0, n - 1):
            outs[k][...] = jnp.zeros_like(outs[k])
        outs[k][some, :] = mixed_all[at, :]


VMEM = pl.BlockSpec(memory_space=pltpu.VMEM)


def prepare(tokens, norm_gain, group_prob, route_logits, expert_ids):
    rows, model = tokens.shape
    return pl.pallas_call(
        prepare_kernel,
        out_shape=[jax.ShapeDtypeStruct((rows, model + LANES), jnp.bfloat16)] * 2,
        in_specs=[VMEM] * 5,
        out_specs=[VMEM] * 2,
        name="prepare",
    )(tokens, norm_gain[None, :], group_prob[None, :], route_logits.T, expert_ids.T)


def expert(units, own, other):
    n = len(units)
    rows, width = units[0].shape
    model = width - LANES
    total = (n - 1) * rows
    params = pltpu.CompilerParams(vmem_limit_bytes=20 * 1024 * 1024)
    whole = jax.ShapeDtypeStruct((total, model), jnp.bfloat16)
    held = pl.pallas_call(
        functools.partial(first_kernel, n),
        out_shape=[whole, jax.ShapeDtypeStruct((total, LANES), jnp.float32), whole],
        in_specs=[VMEM] * (n + 3),
        out_specs=[VMEM] * 3,
        compiler_params=params,
        name="first",
    )(*units, *other)
    return pl.pallas_call(
        functools.partial(second_kernel, n),
        out_shape=[jax.ShapeDtypeStruct((rows, model), jnp.bfloat16)] * n,
        in_specs=[VMEM] * 6,
        out_specs=[VMEM] * n,
        scratch_shapes=[pltpu.VMEM((total, model), jnp.bfloat16)],
        compiler_params=params,
        name="second",
    )(*held, *own)


def turned(array, shift):
    n, cores = lax.axis_size("ep"), lax.axis_size("tp")
    pairs = []
    for i in range(n):
        for core in range(cores):
            to = (i + (shift if core == 0 else -shift)) % n
            pairs.append((i * cores + core, to * cores + core))
    return lax.ppermute(array, ("ep", "tp"), pairs)


def swapped(array):
    return lax.ppermute(array, "tp", [(0, 1), (1, 0)])


def added(*parts):
    total = parts[0].astype(jnp.float32)
    for part in parts[1:]:
        total = total + part.astype(jnp.float32)
    return total.astype(jnp.bfloat16)


def gather(unit):
    held = {0: unit}
    for at in GATHER_ORDER:
        held[at] = turned(held[GATHER[at - 1]], at - GATHER[at - 1])
    return [held[at] for at in range(LAST + 1)]


def combine(outs):
    parts = {at: [out] for at, out in enumerate(outs)}
    for at in COMBINE_ORDER:
        whole = added(*parts[at]) if len(parts[at]) > 1 else outs[at]
        parts[COMBINE[at - 1]].append(turned(whole, COMBINE[at - 1] - at))
    return added(*parts[0])


def shards(tokens, norm_gain, group_prob, route_logits, expert_ids, w_gate, w_up, w_down):
    own, other = (w_gate, w_up, w_down), []
    for w in own:
        other.append(swapped(w))
    unit, kept = prepare(tokens, norm_gain, group_prob, route_logits, expert_ids)
    units = gather(unit)
    mixed = combine(expert([kept, *units[1:]], own, other))
    return added(mixed, swapped(mixed))


def solution(mesh):
    in_specs = (
        P(("grp", "ep"), None),
        P(),
        P(("grp", "ep")),
        P(("grp", "ep"), None),
        P(("grp", "ep"), None),
        P("ep", None, "tp"),
        P("ep", None, "tp"),
        P("ep", "tp", None),
    )
    out_specs = P(("grp", "ep"), None)
    return jax.shard_map(
        shards, mesh=mesh, in_specs=in_specs, out_specs=out_specs, check_vma=False
    )
```

```python
import functools

import jax
import jax.numpy as jnp
from jax import lax
from jax.experimental import pallas as pl
from jax.experimental.pallas import tpu as pltpu
from jax.sharding import PartitionSpec as P


LANES = 128
GROUPS = 2
GATHER = (0, 1, 0, 3, 4, 0, 6, 6, 8, 6, 10, 11, 10, 13, 13, 15)
GATHER_ORDER = (6, 1, 3, 10, 8, 4, 7, 13, 11, 5, 2, 15, 14, 12, 9, 16)
COMBINE = (0, 1, 0, 1, 4, 4, 0, 7, 7, 9, 7, 11, 11, 11, 14, 14)
COMBINE_ORDER = (16, 15, 13, 10, 14, 12, 9, 6, 5, 11, 8, 3, 4, 2, 7, 1)
LAST = len(GATHER)


def own_group():
    return lax.axis_index("ep") // (lax.axis_size("ep") // GROUPS)


def turned_dot(a, b):
    return lax.dot_general(a, b, (((1,), (1,)), ((), ())), preferred_element_type=jnp.float32)


def prepare_kernel(tokens, gain, prob, logits, ids, unit, kept, back):
    rows, model = tokens.shape
    width = unit.shape[1]
    half = rows // GROUPS
    values = tokens[...].astype(jnp.float32)
    scale = lax.rsqrt(jnp.mean(values * values, axis=-1, keepdims=True) + 1e-06)
    normed = (values * scale * gain[...]).astype(jnp.bfloat16)
    expw = jnp.exp(logits[...])
    route_w = prob[...] * expw / jnp.sum(expw, axis=0, keepdims=True)
    picks, count = expw.shape
    experts = lax.axis_size("ep")
    expert = lax.broadcasted_iota(jnp.int32, (experts, count), 0)
    dense = jnp.zeros((experts, count), jnp.float32)
    for k in range(picks):
        dense += jnp.where(ids[k : k + 1, :] == expert, route_w[k : k + 1, :], 0.0)
    high = dense.astype(jnp.bfloat16).astype(jnp.float32)
    low = dense - high
    table = jnp.concatenate(
        [high, low, jnp.zeros((width - model - 2 * experts, count), jnp.float32)], axis=0
    ).astype(jnp.bfloat16)
    row = lax.broadcasted_iota(jnp.int32, (rows, count), 0)
    column = lax.broadcasted_iota(jnp.int32, (rows, count), 1)
    late = jnp.broadcast_to(ids[:1, :] >= experts // GROUPS, (rows, count))
    earlier = (row < column).astype(jnp.bfloat16)
    before = jnp.dot(
        late.astype(jnp.bfloat16), earlier, preferred_element_type=jnp.float32
    ).astype(jnp.int32)
    place = jnp.where(late, half + before, column - before)
    chosen = (place == row).astype(jnp.bfloat16)
    unit[:, :model] = jnp.dot(
        chosen, normed, preferred_element_type=jnp.float32
    ).astype(jnp.bfloat16)
    unit[:, model:] = turned_dot(chosen, table).astype(jnp.bfloat16)
    kept[...] = unit[pl.ds(pl.multiple_of(own_group() * half, half), half), :]
    back[...] = turned_dot((row == column).astype(jnp.bfloat16), chosen)


def block(x, gate_w, up_w, down_w):
    gate = jnp.dot(x, gate_w[0], preferred_element_type=jnp.float32)
    up = jnp.dot(x, up_w[0], preferred_element_type=jnp.float32)
    act = (gate / (1.0 + jnp.exp(-gate)) * up).astype(jnp.bfloat16)
    return jnp.dot(act, down_w[0], preferred_element_type=jnp.float32).astype(jnp.bfloat16)


def first_kernel(n, *refs):
    units, other, (rows_all, weight_all, part_all) = refs[:n], refs[n : n + 3], refs[n + 3 :]
    half, _ = units[0].shape
    model = rows_all.shape[1]
    me, core = lax.axis_index("ep"), lax.axis_index("tp")
    experts = lax.axis_size("ep")
    group = own_group()
    for k, unit in enumerate(units):
        if unit.shape[0] == half:
            some = slice(None)
        else:
            some = pl.ds(pl.multiple_of(group * half, half), half)
        at = slice(k * half, (k + 1) * half)
        rows_all[at, :] = unit[some, :model]
        table = unit[some, model:].astype(jnp.float32)
        lane = lax.broadcasted_iota(jnp.int32, table.shape, 1)
        mine = (lane == me) | (lane == me + experts)
        if k in (0, n - 1):
            mine = mine & (core == (0 if k == 0 else 1))
        taken = jnp.where(mine, table, 0.0)
        weight_all[at, :] = jnp.broadcast_to(jnp.sum(taken, axis=1, keepdims=True), table.shape)
    part_all[...] = block(rows_all[...], *other)


def second_kernel(n, *refs):
    (rows_all, weight_all, part_all, *own), outs = refs[:6], refs[6:]
    half = outs[0].shape[0]
    part = block(rows_all[...], *own).astype(jnp.float32)
    total = (part_all[...].astype(jnp.float32) + part).astype(jnp.bfloat16)
    weighted = (total.astype(jnp.float32) * weight_all[:, :1]).astype(jnp.bfloat16)
    for k in range(n):
        outs[k][...] = weighted[k * half : (k + 1) * half]


VMEM = pl.BlockSpec(memory_space=pltpu.VMEM)


def prepare(tokens, norm_gain, group_prob, route_logits, expert_ids):
    rows, model = tokens.shape
    width = model + LANES
    return pl.pallas_call(
        prepare_kernel,
        out_shape=[
            jax.ShapeDtypeStruct((rows, width), jnp.bfloat16),
            jax.ShapeDtypeStruct((rows // GROUPS, width), jnp.bfloat16),
            jax.ShapeDtypeStruct((rows, rows), jnp.float32),
        ],
        in_specs=[VMEM] * 5,
        out_specs=[VMEM] * 3,
        name="prepare",
    )(tokens, norm_gain[None, :], group_prob[None, :], route_logits.T, expert_ids.T)


def expert(units, own, other):
    n = len(units)
    half, width = units[0].shape
    model = width - LANES
    total = n * half
    params = pltpu.CompilerParams(vmem_limit_bytes=20 * 1024 * 1024)
    whole = jax.ShapeDtypeStruct((total, model), jnp.bfloat16)
    held = pl.pallas_call(
        functools.partial(first_kernel, n),
        out_shape=[whole, jax.ShapeDtypeStruct((total, LANES), jnp.float32), whole],
        in_specs=[VMEM] * (n + 3),
        out_specs=[VMEM] * 3,
        compiler_params=params,
        name="first",
    )(*units, *other)
    return pl.pallas_call(
        functools.partial(second_kernel, n),
        out_shape=[jax.ShapeDtypeStruct((half, model), jnp.bfloat16)] * n,
        in_specs=[VMEM] * 6,
        out_specs=[VMEM] * n,
        compiler_params=params,
        name="second",
    )(*held, *own)


def finish(here, there, back):
    total = (here.astype(jnp.float32) + there.astype(jnp.float32)).astype(jnp.bfloat16)
    return jnp.dot(
        back.astype(jnp.bfloat16), total, preferred_element_type=jnp.float32
    ).astype(jnp.bfloat16)


def turned(array, shift):
    n, cores = lax.axis_size("ep"), lax.axis_size("tp")
    pairs = []
    for i in range(n):
        for core in range(cores):
            to = (i + (shift if core == 0 else -shift)) % n
            pairs.append((i * cores + core, to * cores + core))
    return lax.ppermute(array, ("ep", "tp"), pairs)


def swapped(array):
    return lax.ppermute(array, "tp", [(0, 1), (1, 0)])


def node_kernel(distances, *refs):
    *parts, out, total = refs
    half = out.shape[0] // GROUPS
    n = lax.axis_size("ep")
    me, side = lax.axis_index("ep"), 1 - 2 * lax.axis_index("tp")
    total[...] = jnp.zeros_like(total)
    for part, distance in zip(parts, distances):
        values = part[...].astype(jnp.float32)
        if distance is None:
            total[...] += values
        else:
            group = lax.rem(me + side * distance + n, n) // (n // GROUPS)
            total[pl.ds(pl.multiple_of(group * half, half), half), :] += values
    out[...] = total[...].astype(out.dtype)


def added(parts):
    arrays, distances = zip(*parts)
    half, model = arrays[0].shape
    shape = (GROUPS * half, model)
    return pl.pallas_call(
        functools.partial(node_kernel, distances),
        out_shape=jax.ShapeDtypeStruct(shape, jnp.bfloat16),
        in_specs=[VMEM] * len(arrays),
        out_specs=VMEM,
        scratch_shapes=[pltpu.VMEM(shape, jnp.float32)],
        compiler_params=pltpu.CompilerParams(vmem_limit_bytes=8 * 1024 * 1024),
        name="node",
    )(*arrays)


def gather(unit):
    held = {0: unit}
    for at in GATHER_ORDER:
        by = GATHER[at - 1]
        held[at] = turned(held[by], at - by)
    return [held[at] for at in range(LAST + 1)]


def combine(outs):
    parts = {at: [(out, 0)] for at, out in enumerate(outs)}
    for at in COMBINE_ORDER:
        by = COMBINE[at - 1]
        sent = added(parts[at]) if at in COMBINE else outs[at]
        came = turned(sent, by - at)
        parts[by].append((came, None if at in COMBINE else at - by))
    return added(parts[0])


def shards(tokens, norm_gain, group_prob, route_logits, expert_ids, w_gate, w_up, w_down):
    own, other = (w_gate, w_up, w_down), []
    for w in own:
        other.append(swapped(w))
    unit, kept, back = prepare(tokens, norm_gain, group_prob, route_logits, expert_ids)
    units = gather(unit)
    mixed = combine(expert([kept, *units[1:]], own, other))
    return finish(mixed, swapped(mixed), back)


def solution(mesh):
    in_specs = (
        P(("grp", "ep"), None),
        P(),
        P(("grp", "ep")),
        P(("grp", "ep"), None),
        P(("grp", "ep"), None),
        P("ep", None, "tp"),
        P("ep", None, "tp"),
        P("ep", "tp", None),
    )
    out_specs = P(("grp", "ep"), None)
    return jax.shard_map(
        shards, mesh=mesh, in_specs=in_specs, out_specs=out_specs, check_vma=False
    )
```

```python
import functools

import jax
import jax.numpy as jnp
from jax import lax
from jax.experimental import pallas as pl
from jax.experimental.pallas import tpu as pltpu
from jax.sharding import PartitionSpec as P


LANES = 128
GROUPS = 2
GATHER = (0, 1, 0, 3, 4, 0, 6, 6, 8, 6, 10, 11, 10, 13, 13, 15)
GATHER_ORDER = (6, 1, 3, 10, 8, 4, 7, 13, 11, 5, 2, 15, 14, 12, 9, 16)
COMBINE = (0, 1, 0, 1, 4, 4, 0, 7, 7, 9, 7, 11, 11, 11, 14, 14)
COMBINE_ORDER = (16, 15, 13, 10, 14, 12, 9, 6, 5, 11, 8, 3, 4, 2, 7, 1)
LAST = len(GATHER)


def own_group():
    return lax.axis_index("ep") // (lax.axis_size("ep") // GROUPS)


def turned_dot(a, b):
    return lax.dot_general(a, b, (((1,), (1,)), ((), ())), preferred_element_type=jnp.float32)


def prepare_kernel(tokens, gain, prob, logits, ids, unit, kept, back):
    rows, model = tokens.shape
    width = unit.shape[1]
    half = rows // GROUPS
    values = tokens[...].astype(jnp.float32)
    scale = lax.rsqrt(jnp.mean(values * values, axis=-1, keepdims=True) + 1e-06)
    normed = (values * scale * gain[...]).astype(jnp.bfloat16)
    expw = jnp.exp(logits[...])
    route_w = prob[...] * expw / jnp.sum(expw, axis=0, keepdims=True)
    picks, count = expw.shape
    experts = lax.axis_size("ep")
    expert = lax.broadcasted_iota(jnp.int32, (experts, count), 0)
    dense = jnp.zeros((experts, count), jnp.float32)
    for k in range(picks):
        dense += jnp.where(ids[k : k + 1, :] == expert, route_w[k : k + 1, :], 0.0)
    high = dense.astype(jnp.bfloat16).astype(jnp.float32)
    low = dense - high
    table = jnp.concatenate(
        [high, low, jnp.zeros((width - model - 2 * experts, count), jnp.float32)], axis=0
    ).astype(jnp.bfloat16)
    row = lax.broadcasted_iota(jnp.int32, (rows, count), 0)
    column = lax.broadcasted_iota(jnp.int32, (rows, count), 1)
    late = jnp.broadcast_to(ids[:1, :] >= experts // GROUPS, (rows, count))
    earlier = (row < column).astype(jnp.bfloat16)
    before = jnp.dot(
        late.astype(jnp.bfloat16), earlier, preferred_element_type=jnp.float32
    ).astype(jnp.int32)
    place = jnp.where(late, half + before, column - before)
    chosen = (place == row).astype(jnp.bfloat16)
    unit[:, :model] = jnp.dot(
        chosen, normed, preferred_element_type=jnp.float32
    ).astype(jnp.bfloat16)
    unit[:, model:] = turned_dot(chosen, table).astype(jnp.bfloat16)
    kept[...] = unit[pl.ds(pl.multiple_of(own_group() * half, half), half), :]
    back[...] = turned_dot((row == column).astype(jnp.bfloat16), chosen)


def block(x, gate_w, up_w, down_w):
    gate = jnp.dot(x, gate_w[0], preferred_element_type=jnp.float32)
    up = jnp.dot(x, up_w[0], preferred_element_type=jnp.float32)
    act = (gate / (1.0 + jnp.exp(-gate)) * up).astype(jnp.bfloat16)
    return jnp.dot(act, down_w[0], preferred_element_type=jnp.float32).astype(jnp.bfloat16)


def first_kernel(n, *refs):
    units, other, (rows_all, weight_all, part_all) = refs[:n], refs[n : n + 3], refs[n + 3 :]
    half, _ = units[0].shape
    model = rows_all.shape[1]
    me, core = lax.axis_index("ep"), lax.axis_index("tp")
    experts = lax.axis_size("ep")
    group = own_group()
    for k, unit in enumerate(units):
        if unit.shape[0] == half:
            some = slice(None)
        else:
            some = pl.ds(pl.multiple_of(group * half, half), half)
        at = slice(k * half, (k + 1) * half)
        rows_all[at, :] = unit[some, :model]
        table = unit[some, model:].astype(jnp.float32)
        lane = lax.broadcasted_iota(jnp.int32, table.shape, 1)
        mine = (lane == me) | (lane == me + experts)
        if k in (0, n - 1):
            mine = mine & (core == (0 if k == 0 else 1))
        taken = jnp.where(mine, table, 0.0)
        weight_all[at, :] = jnp.broadcast_to(jnp.sum(taken, axis=1, keepdims=True), table.shape)
    part_all[...] = block(rows_all[...], *other)


def second_kernel(n, *refs):
    (rows_all, weight_all, part_all, *own), outs = refs[:6], refs[6:]
    half = outs[0].shape[0]
    part = block(rows_all[...], *own).astype(jnp.float32)
    total = (part_all[...].astype(jnp.float32) + part).astype(jnp.bfloat16)
    weighted = (total.astype(jnp.float32) * weight_all[:, :1]).astype(jnp.bfloat16)
    for k in range(n):
        outs[k][...] = weighted[k * half : (k + 1) * half]


VMEM = pl.BlockSpec(memory_space=pltpu.VMEM)


def prepare(tokens, norm_gain, group_prob, route_logits, expert_ids):
    rows, model = tokens.shape
    width = model + LANES
    return pl.pallas_call(
        prepare_kernel,
        out_shape=[
            jax.ShapeDtypeStruct((rows, width), jnp.bfloat16),
            jax.ShapeDtypeStruct((rows // GROUPS, width), jnp.bfloat16),
            jax.ShapeDtypeStruct((rows, rows), jnp.float32),
        ],
        in_specs=[VMEM] * 5,
        out_specs=[VMEM] * 3,
        name="prepare",
    )(tokens, norm_gain[None, :], group_prob[None, :], route_logits.T, expert_ids.T)


def hold_kernel(source, out):
    out[...] = source[...]


def hold(array):
    return pl.pallas_call(
        hold_kernel,
        out_shape=jax.ShapeDtypeStruct(array.shape, array.dtype),
        in_specs=[VMEM],
        out_specs=VMEM,
        compiler_params=pltpu.CompilerParams(vmem_limit_bytes=8 * 1024 * 1024),
        name="hold",
    )(array)


def expert(units, own, other):
    n = len(units)
    half, width = units[0].shape
    model = width - LANES
    total = n * half
    params = pltpu.CompilerParams(vmem_limit_bytes=20 * 1024 * 1024)
    whole = jax.ShapeDtypeStruct((total, model), jnp.bfloat16)
    held = pl.pallas_call(
        functools.partial(first_kernel, n),
        out_shape=[whole, jax.ShapeDtypeStruct((total, LANES), jnp.float32), whole],
        in_specs=[VMEM] * (n + 3),
        out_specs=[VMEM] * 3,
        compiler_params=params,
        name="first",
    )(*units, *other)
    return pl.pallas_call(
        functools.partial(second_kernel, n),
        out_shape=[jax.ShapeDtypeStruct((half, model), jnp.bfloat16)] * n,
        in_specs=[VMEM] * 6,
        out_specs=[VMEM] * n,
        compiler_params=params,
        name="second",
    )(*held, *own)


def finish(here, there, back):
    total = (here.astype(jnp.float32) + there.astype(jnp.float32)).astype(jnp.bfloat16)
    return jnp.dot(
        back.astype(jnp.bfloat16), total, preferred_element_type=jnp.float32
    ).astype(jnp.bfloat16)


def turned(array, shift):
    n, cores = lax.axis_size("ep"), lax.axis_size("tp")
    pairs = []
    for i in range(n):
        for core in range(cores):
            to = (i + (shift if core == 0 else -shift)) % n
            pairs.append((i * cores + core, to * cores + core))
    return lax.ppermute(array, ("ep", "tp"), pairs)


def swapped(array):
    return lax.ppermute(array, "tp", [(0, 1), (1, 0)])


def node_kernel(distances, *refs):
    *parts, out, total = refs
    half = out.shape[0] // GROUPS
    n = lax.axis_size("ep")
    me, side = lax.axis_index("ep"), 1 - 2 * lax.axis_index("tp")
    total[...] = jnp.zeros_like(total)
    for part, distance in zip(parts, distances):
        values = part[...].astype(jnp.float32)
        if distance is None:
            total[...] += values
        else:
            group = lax.rem(me + side * distance + n, n) // (n // GROUPS)
            total[pl.ds(pl.multiple_of(group * half, half), half), :] += values
    out[...] = total[...].astype(out.dtype)


def added(parts):
    arrays, distances = zip(*parts)
    half, model = arrays[0].shape
    shape = (GROUPS * half, model)
    return pl.pallas_call(
        functools.partial(node_kernel, distances),
        out_shape=jax.ShapeDtypeStruct(shape, jnp.bfloat16),
        in_specs=[VMEM] * len(arrays),
        out_specs=VMEM,
        scratch_shapes=[pltpu.VMEM(shape, jnp.float32)],
        compiler_params=pltpu.CompilerParams(vmem_limit_bytes=8 * 1024 * 1024),
        name="node",
    )(*arrays)


def gather(unit):
    held = {0: unit}
    for at in GATHER_ORDER:
        by = GATHER[at - 1]
        held[at] = turned(held[by], at - by)
    return [held[at] for at in range(LAST + 1)]


def combine(outs):
    parts = {at: [(out, 0)] for at, out in enumerate(outs)}
    for at in COMBINE_ORDER:
        by = COMBINE[at - 1]
        sent = outs[at]
        if at in COMBINE:
            sent = added(parts[at])
        came = turned(sent, by - at)
        parts[by].append((came, None if at in COMBINE else at - by))
    return added(parts[0])


def shards(tokens, norm_gain, group_prob, route_logits, expert_ids, w_gate, w_up, w_down):
    own, other = (w_gate, w_up, w_down), []
    for w in own:
        other.append(swapped(w))
    unit, kept, back = prepare(tokens, norm_gain, group_prob, route_logits, expert_ids)
    units = gather(unit)
    kept = hold(kept)
    mixed = combine(expert([kept, *units[1:]], own, other))
    return finish(mixed, swapped(mixed), back)


def solution(mesh):
    in_specs = (
        P(("grp", "ep"), None),
        P(),
        P(("grp", "ep")),
        P(("grp", "ep"), None),
        P(("grp", "ep"), None),
        P("ep", None, "tp"),
        P("ep", None, "tp"),
        P("ep", "tp", None),
    )
    out_specs = P(("grp", "ep"), None)
    return jax.shard_map(
        shards, mesh=mesh, in_specs=in_specs, out_specs=out_specs, check_vma=False
    )
```

```python
import functools

import jax
import jax.numpy as jnp
from jax import lax
from jax.experimental import pallas as pl
from jax.experimental.pallas import tpu as pltpu
from jax.sharding import PartitionSpec as P


LANES = 128
GROUPS = 2
GATHER = (0, 0, 2, 0, 4, 4, 6, 7, 4, 9, 10, 9, 12, 12, 14, 14)
GATHER_ORDER = (4, 1, 2, 9, 5, 6, 12, 10, 7, 3, 14, 11, 13, 8, 15, 16)
COMBINE = (0, 0, 2, 3, 0, 5, 5, 7, 8, 5, 10, 11, 10, 13, 13, 15)
COMBINE_ORDER = (16, 12, 9, 14, 15, 8, 4, 11, 1, 13, 6, 7, 3, 10, 2, 5)
LAST = len(GATHER)


def own_group():
    return lax.axis_index("ep") // (lax.axis_size("ep") // GROUPS)


def turned_dot(a, b):
    return lax.dot_general(a, b, (((1,), (1,)), ((), ())), preferred_element_type=jnp.float32)


def prepare_kernel(tokens, gain, prob, logits, ids, unit, kept, back):
    rows, model = tokens.shape
    width = unit.shape[1]
    half = rows // GROUPS
    values = tokens[...].astype(jnp.float32)
    scale = lax.rsqrt(jnp.mean(values * values, axis=-1, keepdims=True) + 1e-06)
    normed = (values * scale * gain[...]).astype(jnp.bfloat16)
    expw = jnp.exp(logits[...])
    route_w = prob[...] * expw / jnp.sum(expw, axis=0, keepdims=True)
    picks, count = expw.shape
    experts = lax.axis_size("ep")
    expert = lax.broadcasted_iota(jnp.int32, (experts, count), 0)
    dense = jnp.zeros((experts, count), jnp.float32)
    for k in range(picks):
        dense += jnp.where(ids[k : k + 1, :] == expert, route_w[k : k + 1, :], 0.0)
    high = dense.astype(jnp.bfloat16).astype(jnp.float32)
    low = dense - high
    table = jnp.concatenate(
        [high, low, jnp.zeros((width - model - 2 * experts, count), jnp.float32)], axis=0
    ).astype(jnp.bfloat16)
    row = lax.broadcasted_iota(jnp.int32, (rows, count), 0)
    column = lax.broadcasted_iota(jnp.int32, (rows, count), 1)
    late = jnp.broadcast_to(ids[:1, :] >= experts // GROUPS, (rows, count))
    earlier = (row < column).astype(jnp.bfloat16)
    before = jnp.dot(
        late.astype(jnp.bfloat16), earlier, preferred_element_type=jnp.float32
    ).astype(jnp.int32)
    place = jnp.where(late, half + before, column - before)
    chosen = (place == row).astype(jnp.bfloat16)
    unit[:, :model] = jnp.dot(
        chosen, normed, preferred_element_type=jnp.float32
    ).astype(jnp.bfloat16)
    unit[:, model:] = turned_dot(chosen, table).astype(jnp.bfloat16)
    kept[...] = unit[pl.ds(pl.multiple_of(own_group() * half, half), half), :]
    back[...] = turned_dot((row == column).astype(jnp.bfloat16), chosen)


def block(x, gate_w, up_w, down_w):
    gate = jnp.dot(x, gate_w[0], preferred_element_type=jnp.float32)
    up = jnp.dot(x, up_w[0], preferred_element_type=jnp.float32)
    act = (gate / (1.0 + jnp.exp(-gate)) * up).astype(jnp.bfloat16)
    return jnp.dot(act, down_w[0], preferred_element_type=jnp.float32).astype(jnp.bfloat16)


def first_kernel(n, *refs):
    units, other, (rows_all, weight_all, part_all) = refs[:n], refs[n : n + 3], refs[n + 3 :]
    half, _ = units[0].shape
    model = rows_all.shape[1]
    me, core = lax.axis_index("ep"), lax.axis_index("tp")
    experts = lax.axis_size("ep")
    group = own_group()
    for k, unit in enumerate(units):
        if unit.shape[0] == half:
            some = slice(None)
        else:
            some = pl.ds(pl.multiple_of(group * half, half), half)
        at = slice(k * half, (k + 1) * half)
        rows_all[at, :] = unit[some, :model]
        table = unit[some, model:].astype(jnp.float32)
        lane = lax.broadcasted_iota(jnp.int32, table.shape, 1)
        mine = (lane == me) | (lane == me + experts)
        if k in (0, n - 1):
            mine = mine & (core == (0 if k == 0 else 1))
        taken = jnp.where(mine, table, 0.0)
        weight_all[at, :] = jnp.broadcast_to(jnp.sum(taken, axis=1, keepdims=True), table.shape)
    part_all[...] = block(rows_all[...], *other)


def second_kernel(n, *refs):
    (rows_all, weight_all, part_all, *own), outs = refs[:6], refs[6:]
    half = outs[0].shape[0]
    part = block(rows_all[...], *own).astype(jnp.float32)
    total = (part_all[...].astype(jnp.float32) + part).astype(jnp.bfloat16)
    weighted = (total.astype(jnp.float32) * weight_all[:, :1]).astype(jnp.bfloat16)
    for k in range(n):
        outs[k][...] = weighted[k * half : (k + 1) * half]


VMEM = pl.BlockSpec(memory_space=pltpu.VMEM)


def prepare(tokens, norm_gain, group_prob, route_logits, expert_ids):
    rows, model = tokens.shape
    width = model + LANES
    return pl.pallas_call(
        prepare_kernel,
        out_shape=[
            jax.ShapeDtypeStruct((rows, width), jnp.bfloat16),
            jax.ShapeDtypeStruct((rows // GROUPS, width), jnp.bfloat16),
            jax.ShapeDtypeStruct((rows, rows), jnp.float32),
        ],
        in_specs=[VMEM] * 5,
        out_specs=[VMEM] * 3,
        name="prepare",
    )(tokens, norm_gain[None, :], group_prob[None, :], route_logits.T, expert_ids.T)


def hold_kernel(source, out):
    out[...] = source[...]


def hold(array):
    return pl.pallas_call(
        hold_kernel,
        out_shape=jax.ShapeDtypeStruct(array.shape, array.dtype),
        in_specs=[VMEM],
        out_specs=VMEM,
        compiler_params=pltpu.CompilerParams(vmem_limit_bytes=8 * 1024 * 1024),
        name="hold",
    )(array)


def expert(units, own, other):
    n = len(units)
    half, width = units[0].shape
    model = width - LANES
    total = n * half
    params = pltpu.CompilerParams(vmem_limit_bytes=20 * 1024 * 1024)
    whole = jax.ShapeDtypeStruct((total, model), jnp.bfloat16)
    held = pl.pallas_call(
        functools.partial(first_kernel, n),
        out_shape=[whole, jax.ShapeDtypeStruct((total, LANES), jnp.float32), whole],
        in_specs=[VMEM] * (n + 3),
        out_specs=[VMEM] * 3,
        compiler_params=params,
        name="first",
    )(*units, *other)
    return pl.pallas_call(
        functools.partial(second_kernel, n),
        out_shape=[jax.ShapeDtypeStruct((half, model), jnp.bfloat16)] * n,
        in_specs=[VMEM] * 6,
        out_specs=[VMEM] * n,
        compiler_params=params,
        name="second",
    )(*held, *own)


def finish(here, there, back):
    total = (here.astype(jnp.float32) + there.astype(jnp.float32)).astype(jnp.bfloat16)
    return jnp.dot(
        back.astype(jnp.bfloat16), total, preferred_element_type=jnp.float32
    ).astype(jnp.bfloat16)


def turned(array, shift):
    n, cores = lax.axis_size("ep"), lax.axis_size("tp")
    pairs = []
    for i in range(n):
        for core in range(cores):
            to = (i + (shift if core == 0 else -shift)) % n
            pairs.append((i * cores + core, to * cores + core))
    return lax.ppermute(array, ("ep", "tp"), pairs)


def swapped(array):
    return lax.ppermute(array, "tp", [(0, 1), (1, 0)])


def node_kernel(distances, *refs):
    *parts, out, total = refs
    half = out.shape[0] // GROUPS
    n = lax.axis_size("ep")
    me, side = lax.axis_index("ep"), 1 - 2 * lax.axis_index("tp")
    total[...] = jnp.zeros_like(total)
    for part, distance in zip(parts, distances):
        values = part[...].astype(jnp.float32)
        if distance is None:
            total[...] += values
        else:
            group = lax.rem(me + side * distance + n, n) // (n // GROUPS)
            total[pl.ds(pl.multiple_of(group * half, half), half), :] += values
    out[...] = total[...].astype(out.dtype)


def added(parts):
    arrays, distances = zip(*parts)
    half, model = arrays[0].shape
    shape = (GROUPS * half, model)
    return pl.pallas_call(
        functools.partial(node_kernel, distances),
        out_shape=jax.ShapeDtypeStruct(shape, jnp.bfloat16),
        in_specs=[VMEM] * len(arrays),
        out_specs=VMEM,
        scratch_shapes=[pltpu.VMEM(shape, jnp.float32)],
        compiler_params=pltpu.CompilerParams(vmem_limit_bytes=8 * 1024 * 1024),
        name="node",
    )(*arrays)


def gather(unit):
    held = {0: unit}
    for at in GATHER_ORDER:
        by = GATHER[at - 1]
        held[at] = turned(held[by], at - by)
    return [held[at] for at in range(LAST + 1)]


def combine(outs):
    parts = {at: [(out, 0)] for at, out in enumerate(outs)}
    for at in COMBINE_ORDER:
        by = COMBINE[at - 1]
        sent = outs[at]
        if at in COMBINE:
            sent = added(parts[at])
        came = turned(sent, by - at)
        parts[by].append((came, None if at in COMBINE else at - by))
    return added(parts[0])


def shards(tokens, norm_gain, group_prob, route_logits, expert_ids, w_gate, w_up, w_down):
    own, other = (w_gate, w_up, w_down), []
    for w in own:
        other.append(swapped(w))
    unit, kept, back = prepare(tokens, norm_gain, group_prob, route_logits, expert_ids)
    units = gather(unit)
    kept = hold(kept)
    mixed = combine(expert([kept, *units[1:]], own, other))
    return finish(mixed, swapped(mixed), back)


def solution(mesh):
    in_specs = (
        P(("grp", "ep"), None),
        P(),
        P(("grp", "ep")),
        P(("grp", "ep"), None),
        P(("grp", "ep"), None),
        P("ep", None, "tp"),
        P("ep", None, "tp"),
        P("ep", "tp", None),
    )
    out_specs = P(("grp", "ep"), None)
    return jax.shard_map(
        shards, mesh=mesh, in_specs=in_specs, out_specs=out_specs, check_vma=False
    )
```
